32 devices in a mesh: sp: 8 (over z, x), tp: 4 (over y, core).
Axes of the slice: x: 2, y: 2, z: 4, core: 2. Of those that a mesh axis runs over, the one named last changes fastest.
Arguments:
- residual_in: bfloat16 [2048, 2048], P('sp', 'tp'), may hold values from -6 to 6
- conv_input: bfloat16 [2048, 512], P('sp', 'tp'), may hold values from -6 to 6
- outer_gate: bfloat16 [2048, 512], P('sp', 'tp'), may hold values from -6 to 6
- inner_gate: bfloat16 [2048, 512], P('sp', 'tp'), may hold values from -6 to 6
- documents: int32 [2048], P('sp'), may hold values from 0 to 3, as said below
- conv_taps: float32 [3, 512], P(None, 'tp'), may hold values from -3 to 3
- mixer_gain: float32 [512], replicated, may hold values from 0.1 to 1.9
- output_weight: bfloat16 [512, 2048], P(None, 'tp'), may hold values from -0.25 to 0.25
- ffn_gain: float32 [2048], P('tp'), may hold values from 0.1 to 1.9
- routes: int32 [2048, 2], P('sp'), may hold values from 0 to 7, all different within a row; in each aligned block of 256 rows (0 to 255, 256 to 511, ...) at most 128 rows name the same one
- route_weights: float32 [2048, 2], P('sp'), may hold values from 0.1 to 0.9
- expert_gate: bfloat16 [8, 2048, 3584], P('sp', None, 'tp'), may hold values from -0.125 to 0.125
- expert_up: bfloat16 [8, 2048, 3584], P('sp', None, 'tp'), may hold values from -0.125 to 0.125
- expert_down: bfloat16 [8, 3584, 2048], P('sp', 'tp'), may hold values from -0.09375 to 0.09375
Outputs:
- layer_out: bfloat16 [2048, 2048], P('sp', 'tp')
The draws below stay inside these ranges and needn't reach their ends.
Inputs may be any that keep to these rules, and one draw needn't show every extreme that they name: Document numbers never fall along the positions, and each of the 4 documents occurs. Every document has 256 to 768 positions, and one has exactly 768. `routes`: the two experts of a position differ. Among the 256 positions of one index of sp no expert is named more than 128 times, a bound that some block reaches.
All inputs are finite; a program needn't handle non-finite values.
Results may differ from the reference program's by a relative error of at most 0.0058.
Values may be sent and summed in bfloat16 or wider, within the bound.
A program may use at most 64 MiB of HBM per device.

```python
import math
import jax
import jax.numpy as jnp
import numpy as np
from jax import lax

D = 2048
CH = 512
FE = 3584
TOK_DEV = 256
TOKENS = 2048
EXPERTS = 8
CAP = 128
SEGS = 4
N_SP = 8
N_TP = 4


def draw_documents(key, part):
    half = TOK_DEV // 2
    pick_key = jax.random.fold_in(key, 11)
    shift_key = jax.random.fold_in(key, 23)
    longest = jax.random.randint(pick_key, (), 1, SEGS - 1, dtype=jnp.int32)
    jitter = jax.random.randint(shift_key, (SEGS - 1,), -half, half + 1, dtype=jnp.int32)
    number = jnp.arange(1, SEGS, dtype=jnp.int32)
    jitter = jnp.where(number == longest, -half, jitter)
    jitter = jnp.where(number == longest + 1, half, jitter)
    starts = number * (2 * TOK_DEV) + jitter
    places = jnp.arange(TOKENS, dtype=jnp.int32)
    return jnp.sum((places[:, None] >= starts[None, :]).astype(jnp.int32), axis=1).astype(jnp.int32)


def shard_levels(rng, extent, cuts, low, largest):
    def one(axis_at, blocks):
        steps = jax.random.uniform(jax.random.fold_in(jax.random.fold_in(rng, 6), axis_at), (blocks,), jnp.float32, low / len(cuts), largest / len(cuts))
        return jnp.repeat(jnp.exp(steps), extent[axis_at] // blocks).reshape((-1,) + (1,) * (len(extent) - axis_at - 1))

    gain = one(*cuts[0])
    for cut in cuts[1:]:
        gain = gain * one(*cut)
    return gain


def deal_out(key, own, number, rows, amount, top, bound, lean):
    sequence = jax.random.permutation(key, amount)
    heavy_load, usual = shares(amount, rows * top, bound, lean, True), shares(amount, rows * top, bound, lean, False)
    places = jnp.arange(amount)

    def named(tallies, offset_by):
        used = int((tallies > 0).sum())
        fixed = max(1, used // 4)
        shifted = fixed + (places - fixed + offset_by * (used - fixed)) % max(1, amount - fixed)
        return jnp.zeros((amount,), jnp.int32).at[sequence[jnp.where(places < fixed, places, shifted)]].set(jnp.asarray(tallies, jnp.int32))

    tallies = jnp.where(number % 4 == 0, named(heavy_load, number // 4), named(usual, number - number // 4 - 1))
    mixed = jax.random.permutation(jax.random.fold_in(own, 3), amount)
    source_of, taker = mixed[0:amount // 2 * 2:2], mixed[1:amount // 2 * 2:2]
    slack = jnp.minimum(tallies[source_of] - 1, bound - tallies[taker]) // 2
    slack = jnp.where((source_of == sequence[0]) | (taker == sequence[0]) | (tallies[taker] == 0), 0, jnp.maximum(slack, 0))
    shifted = jax.random.randint(jax.random.fold_in(own, 4), (amount // 2,), 0, 1 << 20) % (slack + 1)
    tallies = tallies.at[source_of].add(-shifted).at[taker].add(shifted)
    labels = jnp.searchsorted(jnp.cumsum(tallies), jnp.arange(rows * top), side="right").astype(jnp.int32)
    grid = labels.reshape(top, rows).T
    grid = grid[jax.random.permutation(jax.random.fold_in(own, 1), rows)]
    offset_by = jax.random.randint(jax.random.fold_in(own, 2), (rows, 1), 0, top)
    return jnp.take_along_axis(grid, (jnp.arange(top)[None, :] + offset_by) % top, axis=1)


def shares(count, total, limit, skew, full):
    portions = [(1 << 20) // math.isqrt(rank ** skew) + 1 for rank in range(1, count + 1)]
    largest = limit if full else min(limit, max(-(-total // count), total * portions[0] // sum(portions)))
    least = 1 if total - largest >= count - 1 else 0
    holding, rest = [largest] + [least] * (count - 1), total - largest - least * (count - 1)
    while rest > 0:
        movable = [i for i in range(1, count) if holding[i] < largest] or [i for i in range(1, count) if holding[i] < limit]
        whole, left = sum([portions[i] for i in movable]), rest
        for i in movable:
            extra = min(limit - holding[i], max(1, left * portions[i] // whole), rest)
            holding[i] = holding[i] + extra
            rest = rest - extra
    return np.array(holding)


def centred(rng, dims, deviation, limit, pieces=(), kind=jnp.bfloat16):
    array = deviation * jax.random.normal(rng, dims, jnp.float32)
    if pieces:
        array = array * shard_levels(rng, dims, pieces, -0.22, 0.18)
    return jnp.clip(array, -limit, limit).astype(kind)


def setup_inputs(seed: int = 0) -> dict:
    seeds = jax.random.split(jax.random.key(seed), 15)
    residual_in = centred(seeds[0], (TOKENS, D), 1.0, 6.0, ((0, 8), (1, 4)))
    conv_input = centred(seeds[1], (TOKENS, CH), 1.0, 6.0, ((0, 8), (1, 4)))
    outer_gate = centred(seeds[2], (TOKENS, CH), 1.0, 6.0, ((0, 8), (1, 4)))
    inner_gate = centred(seeds[3], (TOKENS, CH), 1.0, 6.0, ((0, 8), (1, 4)))
    documents = draw_documents(jax.random.fold_in(seeds[14], 71), 0)
    conv_taps = centred(seeds[5], (3, CH), 0.6, 3.0, ((1, 4),), jnp.float32)
    mixer_gain = jnp.clip(1.0 + 0.18 * jax.random.normal(seeds[6], (CH,), jnp.float32), 0.1, 1.9)
    output_weight = centred(seeds[7], (CH, D), CH ** -0.5, 0.25, ((1, 4),))
    ffn_gain = jnp.clip(1.0 + 0.18 * jax.random.normal(seeds[8], (D,), jnp.float32), 0.1, 1.9)
    routes_keys = jax.random.split(jax.random.fold_in(seeds[9], 1), TOKENS // TOK_DEV)
    routes_turns = jax.random.permutation(jax.random.fold_in(seeds[9], 3), TOKENS // TOK_DEV)
    routes = jax.vmap(lambda own, number: deal_out(jax.random.fold_in(seeds[9], 2), own, number, TOK_DEV, EXPERTS, 2, CAP, 1))(routes_keys, routes_turns).reshape((TOKENS, 2))
    route_weights = jnp.clip(0.1 + 0.79999997 * jax.random.uniform(seeds[10], (TOKENS, 2), jnp.float32) ** shard_levels(seeds[10], (TOKENS, 2), ((0, 8),), -0.2, 0.2), 0.1, 0.9)
    expert_gate = centred(seeds[11], (EXPERTS, D, FE), D ** -0.5, 0.125, ((0, 8), (2, 4)))
    expert_up = centred(seeds[12], (EXPERTS, D, FE), D ** -0.5, 0.125, ((0, 8), (2, 4)))
    expert_down = centred(seeds[13], (EXPERTS, FE, D), FE ** -0.5, 0.09375, ((0, 8), (1, 4)))
    return {"residual_in": residual_in, "conv_input": conv_input, "outer_gate": outer_gate, "inner_gate": inner_gate, "documents": documents, "conv_taps": conv_taps, "mixer_gain": mixer_gain, "output_weight": output_weight, "ffn_gain": ffn_gain, "routes": routes, "route_weights": route_weights, "expert_gate": expert_gate, "expert_up": expert_up, "expert_down": expert_down}


EPS = 1e-06

def slot_tables(routes, experts, capacity):
    tokens = routes.shape[0]
    flattened = routes.reshape(-1)
    onehot = (flattened[:, None] == jnp.arange(experts, dtype=jnp.int32)[None, :]).astype(jnp.int32)
    earlier = jnp.cumsum(onehot, axis=0) - onehot
    position_in = lax.optimization_barrier(jnp.sum(earlier * onehot, axis=1))
    target = flattened * capacity + position_in
    owners = jnp.full((experts * capacity,), tokens, jnp.int32).at[target].set(jnp.arange(2 * tokens, dtype=jnp.int32) // 2)
    return (target.astype(jnp.int32), owners)

def reference(residual_in, conv_input, outer_gate, inner_gate, documents, conv_taps, mixer_gain, output_weight, ffn_gain, routes, route_weights, expert_gate, expert_up, expert_down):
    conv_value = (inner_gate.astype(jnp.float32) * conv_input.astype(jnp.float32)).astype(jnp.bfloat16)
    values = conv_value.astype(jnp.float32)
    zero_row = jnp.zeros((1, CH), jnp.float32)
    back_one = jnp.concatenate([zero_row, values[:-1]], axis=0)
    back_two = jnp.concatenate([zero_row, zero_row, values[:-2]], axis=0)
    minus = jnp.full((1,), -1, jnp.int32)
    doc_one = jnp.concatenate([minus, documents[:-1]], axis=0)
    doc_two = jnp.concatenate([minus, minus, documents[:-2]], axis=0)
    same_one = (doc_one == documents).astype(jnp.float32)[:, None]
    same_two = (doc_two == documents).astype(jnp.float32)[:, None]
    conv_sum = conv_taps[2] * values + conv_taps[1] * back_one * same_one + conv_taps[0] * back_two * same_two
    mixed = (outer_gate.astype(jnp.float32) * conv_sum).astype(jnp.bfloat16)
    mixed_f = mixed.astype(jnp.float32)
    mix_scale = lax.rsqrt(lax.optimization_barrier(jnp.mean(mixed_f * mixed_f, axis=1)) + EPS)
    mix_scaled = (mixed_f * mixer_gain).astype(jnp.bfloat16)
    projected = jnp.dot(mix_scaled, output_weight, preferred_element_type=jnp.float32)
    hidden_state = residual_in.astype(jnp.float32) + projected * mix_scale[:, None]
    feature_scale = lax.rsqrt(lax.optimization_barrier(jnp.mean(hidden_state * hidden_state, axis=1)) + EPS)
    normed = (hidden_state * feature_scale[:, None] * ffn_gain).astype(jnp.bfloat16)
    blocks = routes.reshape(N_SP, TOK_DEV, 2)
    target, owners = jax.vmap(lambda r: slot_tables(r, EXPERTS, CAP))(blocks)
    offsets = (jnp.arange(N_SP, dtype=jnp.int32) * TOK_DEV)[:, None]
    global_owner = jnp.where(owners == TOK_DEV, TOKENS, owners + offsets).astype(jnp.int32)
    expert_index = global_owner.reshape(N_SP, EXPERTS, CAP).transpose(1, 0, 2).reshape(EXPERTS, N_SP * CAP)
    padded = jnp.concatenate([normed, jnp.zeros((1, D), jnp.bfloat16)], axis=0)
    quarter = FE // N_TP

    def one_expert(inputs):
        gate_w, up_w, down_w, index_rows = inputs
        rows = padded[index_rows]
        gate = jnp.dot(rows, gate_w, preferred_element_type=jnp.float32)
        upper = jnp.dot(rows, up_w, preferred_element_type=jnp.float32)
        act = (jax.nn.silu(gate) * upper).astype(jnp.bfloat16)
        total = jnp.zeros((rows.shape[0], D), jnp.float32)
        for block in range(N_TP):
            partial_out = jnp.dot(act[:, block * quarter:(block + 1) * quarter], down_w[block * quarter:(block + 1) * quarter], preferred_element_type=jnp.float32)
            total = total + partial_out.astype(jnp.bfloat16).astype(jnp.float32)
        return total.astype(jnp.bfloat16)
    expert_rows = lax.map(one_expert, (expert_gate, expert_up, expert_down, expert_index))
    expert_of = target // CAP
    slot_of = target % CAP
    global_slot = expert_of * (N_SP * CAP) + (jnp.arange(N_SP, dtype=jnp.int32) * CAP)[:, None] + slot_of
    picked = expert_rows.reshape(EXPERTS * N_SP * CAP, D)[global_slot.reshape(-1)]
    picked = picked.astype(jnp.float32).reshape(TOKENS, 2, D)
    routed = lax.optimization_barrier(jnp.sum(picked * route_weights[:, :, None], axis=1))
    return (hidden_state + routed).astype(jnp.bfloat16)
```

```python
import functools

import jax
import jax.numpy as jnp
from jax import lax
from jax.experimental import pallas as pl
from jax.experimental.pallas import tpu as pltpu
from jax.sharding import PartitionSpec as P

EPS = 1e-06
MESH = pl.DeviceIdType.MESH


def from_behind(block, axis, distance):
    devices = range(lax.axis_size(axis))
    route = [(i - distance, i) for i in devices if i - distance in devices]
    return lax.ppermute(block, axis, route)


def slot_tables(routes, experts, capacity):
    tokens = routes.shape[0]
    flattened = routes.reshape(-1)
    onehot = (flattened[:, None] == jnp.arange(experts, dtype=jnp.int32)[None, :]).astype(jnp.int32)
    earlier = jnp.cumsum(onehot, axis=0) - onehot
    position_in = jnp.sum(earlier * onehot, axis=1)
    target = flattened * capacity + position_in
    owners = (
        jnp.full((experts * capacity,), tokens, jnp.int32)
        .at[target]
        .set(jnp.arange(2 * tokens, dtype=jnp.int32) // 2)
    )
    return (target, owners)


def expert_kernel(
    n,
    group,
    out_ref_in,
    gate_hbm,
    up_hbm,
    down_hbm,
    returned,
    wg,
    wu,
    wd,
    arrived,
    act,
    msend,
    mrecv,
    mine,
    ysend,
    yrecv,
    mine2,
    rsend,
    w_sem,
    a2a_s,
    a2a_r,
    agy_s,
    agy_r,
    agm_s,
    agm_r,
    agf_s,
    agf_r,
    rsm_s,
    rsm_r,
    rsy_s,
    rsy_r,
    ret_s,
    ret_r,
):
    outgoing = out_ref_in
    me = lax.axis_index("sp")
    t = lax.axis_index("tp")
    a = t // 2
    b = t % 2
    mate = 2 * a + (1 - b)
    partner = 2 * (1 - a) + b
    cap, lf = outgoing.shape[1], outgoing.shape[2]
    hidden = wg.shape[1]
    rows = group * cap
    steps = n // group

    loads = [
        pltpu.make_async_copy(gate_hbm.at[0], wg, w_sem.at[0]),
        pltpu.make_async_copy(up_hbm.at[0], wu, w_sem.at[1]),
        pltpu.make_async_copy(down_hbm.at[0], wd, w_sem.at[2]),
    ]
    for load in loads:
        load.start()

    barrier = pltpu.get_barrier_semaphore()

    def greet(p, c):
        pl.semaphore_signal(
            barrier, inc=1, device_id={"sp": (me + p) % n}, device_id_type=MESH
        )
        return c

    lax.fori_loop(1, n, greet, 0)
    for other in (mate, partner):
        pl.semaphore_signal(barrier, inc=1, device_id={"tp": other}, device_id_type=MESH)
    pl.semaphore_wait(barrier, n + 1)

    def remote(src, dst, s, r, dev):
        return pltpu.make_async_remote_copy(
            src_ref=src, dst_ref=dst, send_sem=s, recv_sem=r, device_id=dev, device_id_type=MESH
        )

    def span(p):
        return pl.ds(pl.multiple_of(p * cap, cap), cap)

    def span_g(i):
        return pl.ds(pl.multiple_of(i * rows, rows), rows)

    def a2a(p):
        return remote(
            outgoing.at[(me + p) % n],
            arrived.at[t, span(p)],
            a2a_s.at[p],
            a2a_r.at[p],
            {"sp": (me + p) % n},
        )

    def slab(p):
        return arrived.at[t, span(p)]

    def agy(p):
        return remote(slab(p), slab(p), agy_s.at[p], agy_r.at[p], {"tp": partner})

    def agm(p):
        return remote(slab(p), slab(p), agm_s.at[p], agm_r.at[p], {"tp": mate})

    def agf(p):
        piece = arrived.at[partner, span(p)]
        return remote(piece, piece, agf_s.at[p], agf_r.at[p], {"tp": mate})

    def rsm(i):
        return remote(msend.at[i], mrecv.at[i], rsm_s.at[i], rsm_r.at[i], {"tp": mate})

    def rsy(i):
        return remote(ysend.at[i], yrecv.at[i], rsy_s.at[i], rsy_r.at[i], {"tp": partner})

    def ret(p):
        return remote(
            rsend.at[span(p)],
            returned.at[me],
            ret_s.at[p],
            ret_r.at[p],
            {"sp": (me + n - p) % n},
        )

    def each(low, high, f):
        def one(p, c):
            f(p)
            return c

        lax.fori_loop(low, high, one, 0)

    each(1, n, lambda p: a2a(p).start())
    arrived[t, pl.ds(0, cap), :] = outgoing[me]

    def spread(p):
        @pl.when(p > 0)
        def _():
            a2a(p).wait_recv()

        agy(p).start()
        agm(p).start()

    def relay(p):
        agy(p).wait_recv()
        agf(p).start()

    def settle(p):
        agm(p).wait_recv()
        agf(p).wait_recv()

    def over_group(i, f):
        each(i * group, (i + 1) * group, f)

    def reduce_mate(i):
        rsm(i).wait_recv()
        ysend[i] = (mine[1 - a] + mrecv[i, 1 - a].astype(jnp.float32)).astype(jnp.bfloat16)
        rsy(i).start()
        mine2[...] = mine[a] + mrecv[i, a].astype(jnp.float32)

    def reduce_partner(i):
        rsy(i).wait_recv()
        rsend[span_g(i), :] = (mine2[...] + yrecv[i].astype(jnp.float32)).astype(jnp.bfloat16)

        def back(p):
            @pl.when(p > 0)
            def _():
                ret(p).start()

        over_group(i, back)

    def compute(i):
        def hidden_tile(j, c):
            cols = pl.ds(pl.multiple_of(j * 128, 128), 128)
            both = None
            for q in range(4):
                deep = slice(q * lf, (q + 1) * lf)
                w = jnp.concatenate([wg[deep, cols], wu[deep, cols]], axis=1)
                part = jnp.dot(arrived[q, span_g(i), :], w, preferred_element_type=jnp.float32)
                both = part if both is None else both + part
            g = both[:, :128]
            act[:, cols] = (g * jax.nn.sigmoid(g) * both[:, 128:]).astype(jnp.bfloat16)
            return c

        lax.fori_loop(0, hidden // 128, hidden_tile, 0)
        for qa in range(2):
            far = pl.ds(pl.multiple_of((2 * qa + 1 - b) * lf, lf), lf)
            msend[i, qa] = jnp.dot(
                act[...], wd[:, far], preferred_element_type=jnp.float32
            ).astype(jnp.bfloat16)
        rsm(i).start()
        for qa in range(2):
            near = pl.ds(pl.multiple_of((2 * qa + b) * lf, lf), lf)
            mine[qa] = jnp.dot(act[...], wd[:, near], preferred_element_type=jnp.float32)

    over_group(0, spread)
    for load in loads:
        load.wait()

    def step(i, c):
        @pl.when(i + 1 < steps)
        def _():
            over_group(i + 1, spread)

        over_group(i, relay)

        @pl.when(i > 0)
        def _():
            reduce_mate(i - 1)

        over_group(i, settle)
        compute(i)

        @pl.when(i > 0)
        def _():
            reduce_partner(i - 1)

        return c

    lax.fori_loop(0, steps, step, 0)
    reduce_mate(steps - 1)
    reduce_partner(steps - 1)
    returned[me] = rsend[pl.ds(0, cap), :]

    def finish(p):
        agy(p).wait_send()
        agm(p).wait_send()
        agf(p).wait_send()

        @pl.when(p > 0)
        def _():
            a2a(p).wait_send()
            ret(p).wait_send()
            ret(p).wait_recv()

    each(0, n, finish)

    def finish_group(i):
        rsm(i).wait_send()
        rsy(i).wait_send()

    each(0, steps, finish_group)


def expert_exchange(outgoing, expert_gate, expert_up, expert_down):
    n, cap, lf = outgoing.shape
    hidden = expert_gate.shape[2]
    width = expert_gate.shape[1]
    group = max(1, min(n, 256 // cap))
    rows, steps = group * cap, n // group
    bf, f32 = jnp.bfloat16, jnp.float32
    dma = pltpu.SemaphoreType.DMA
    return pl.pallas_call(
        functools.partial(expert_kernel, n, group),
        out_shape=jax.ShapeDtypeStruct((n, cap, lf), bf),
        in_specs=[pl.BlockSpec(memory_space=pltpu.VMEM)]
        + [pl.BlockSpec(memory_space=pl.ANY)] * 3,
        out_specs=pl.BlockSpec(memory_space=pltpu.VMEM),
        scratch_shapes=[
            pltpu.VMEM((width, hidden), bf),
            pltpu.VMEM((width, hidden), bf),
            pltpu.VMEM((hidden, width), bf),
            pltpu.VMEM((4, n * cap, lf), bf),
            pltpu.VMEM((rows, hidden), bf),
            pltpu.VMEM((steps, 2, rows, lf), bf),
            pltpu.VMEM((steps, 2, rows, lf), bf),
            pltpu.VMEM((2, rows, lf), f32),
            pltpu.VMEM((steps, rows, lf), bf),
            pltpu.VMEM((steps, rows, lf), bf),
            pltpu.VMEM((rows, lf), f32),
            pltpu.VMEM((n * cap, lf), bf),
            dma((3,)),
        ]
        + [dma((n,))] * 8
        + [dma((steps,))] * 4
        + [dma((n,))] * 2,
        compiler_params=pltpu.CompilerParams(
            collective_id=0, has_side_effects=True, vmem_limit_bytes=48 * 1024 * 1024
        ),
        name="expert_exchange",
    )(outgoing, expert_gate, expert_up, expert_down)


def per_device(
    residual_in,
    conv_input,
    outer_gate,
    inner_gate,
    documents,
    conv_taps,
    mixer_gain,
    output_weight,
    ffn_gain,
    routes,
    route_weights,
    expert_gate,
    expert_up,
    expert_down,
):
    tokens_here = residual_in.shape[0]
    local_features = residual_in.shape[1]
    conv_value = (inner_gate.astype(jnp.float32) * conv_input.astype(jnp.float32)).astype(
        jnp.bfloat16
    )
    doc_marks = documents.astype(jnp.bfloat16)
    before_rows, before_docs = from_behind((conv_value[-2:], doc_marks[-2:]), "sp", 1)
    joined_rows = jnp.concatenate([before_rows, conv_value], axis=0).astype(jnp.float32)
    joined_docs = jnp.concatenate([before_docs, doc_marks], axis=0)
    same_one = (joined_docs[1:-1] == doc_marks).astype(jnp.float32)[:, None]
    same_two = (joined_docs[:-2] == doc_marks).astype(jnp.float32)[:, None]
    conv_sum = (
        conv_taps[2] * joined_rows[2:]
        + conv_taps[1] * joined_rows[1:-1] * same_one
        + conv_taps[0] * joined_rows[:-2] * same_two
    )
    mixed = (outer_gate.astype(jnp.float32) * conv_sum).astype(jnp.bfloat16)
    piece_f = lax.all_gather(mixed, "tp", axis=1, tiled=True).astype(jnp.float32)
    scaled = (piece_f * mixer_gain).astype(jnp.bfloat16)
    accum = jnp.dot(scaled, output_weight, preferred_element_type=jnp.float32)
    squares = jnp.sum(piece_f * piece_f, axis=1)
    mix_scale = lax.rsqrt(squares / mixer_gain.shape[0] + EPS)
    hidden_state = residual_in.astype(jnp.float32) + accum * mix_scale[:, None]
    feature_total = lax.psum(jnp.sum(hidden_state * hidden_state, axis=1), "tp")
    model_width = local_features * lax.axis_size("tp")
    normed = (
        hidden_state * lax.rsqrt(feature_total / model_width + EPS)[:, None] * ffn_gain
    ).astype(jnp.bfloat16)
    experts = lax.axis_size("sp") * expert_gate.shape[0]
    capacity = 4 * tokens_here // experts
    target, owners = slot_tables(routes, experts, capacity)
    padded = jnp.concatenate([normed, jnp.zeros((1, local_features), jnp.bfloat16)], axis=0)
    outgoing = padded[owners].reshape(experts, capacity, local_features)
    returned = expert_exchange(outgoing, expert_gate, expert_up, expert_down)
    picked = returned.reshape(experts * capacity, local_features)[target].astype(jnp.float32)
    picked = picked.reshape(tokens_here, 2, local_features)
    routed = jnp.sum(picked * route_weights[:, :, None], axis=1)
    return (hidden_state + routed).astype(jnp.bfloat16)


def solution(mesh):
    placed = (
        P("sp", "tp"),
        P("sp", "tp"),
        P("sp", "tp"),
        P("sp", "tp"),
        P("sp"),
        P(None, "tp"),
        P(),
        P(None, "tp"),
        P("tp"),
        P("sp", None),
        P("sp", None),
        P("sp", None, "tp"),
        P("sp", None, "tp"),
        P("sp", "tp", None),
    )
    return jax.shard_map(
        per_device, mesh=mesh, in_specs=placed, out_specs=P("sp", "tp"), check_vma=False
    )
```

```python
import functools

import jax
import jax.numpy as jnp
from jax import lax
from jax.experimental import pallas as pl
from jax.experimental.pallas import tpu as pltpu
from jax.sharding import PartitionSpec as P

EPS = 1e-06
MESH = pl.DeviceIdType.MESH


def layer_kernel(
    n,
    group,
    residual_hbm,
    conv_input,
    outer_gate,
    inner_gate,
    documents,
    conv_taps,
    mixer_gain,
    ow_hbm,
    ffn_gain,
    routes,
    route_weights,
    gate_hbm,
    up_hbm,
    down_hbm,
    layer_out,
    residual,
    ow,
    halo_conv,
    halo_inner,
    halo_docs,
    joined,
    joined_docs,
    mixbuf,
    totals,
    hidden,
    normed,
    outgoing,
    returned,
    wg,
    wu,
    wd,
    arrived,
    act,
    msend,
    mrecv,
    mine,
    ysend,
    yrecv,
    mine2,
    rsend,
    w_sem,
    a2a_s,
    a2a_r,
    agy_s,
    agy_r,
    agm_s,
    agm_r,
    agf_s,
    agf_r,
    rsm_s,
    rsm_r,
    rsy_s,
    rsy_r,
    ret_s,
    ret_r,
    halo_s,
    halo_r,
    mix_s,
    mix_r,
    tot_s,
    tot_r,
):
    me = lax.axis_index("sp")
    t = lax.axis_index("tp")
    a = t // 2
    b = t % 2
    mate = 2 * a + (1 - b)
    partner = 2 * (1 - a) + b
    across = 2 * (1 - a) + (1 - b)
    cap, lf = outgoing.shape[1], outgoing.shape[2]
    units = wg.shape[1]
    tokens = conv_input.shape[0]
    chans = conv_input.shape[1]
    rows = group * cap
    steps = n // group

    early = [
        pltpu.make_async_copy(ow_hbm, ow, w_sem.at[3]),
        pltpu.make_async_copy(residual_hbm, residual, w_sem.at[4]),
    ]
    loads = [
        pltpu.make_async_copy(gate_hbm.at[0], wg, w_sem.at[0]),
        pltpu.make_async_copy(up_hbm.at[0], wu, w_sem.at[1]),
        pltpu.make_async_copy(down_hbm.at[0], wd, w_sem.at[2]),
    ]
    for load in early + loads:
        load.start()

    barrier = pltpu.get_barrier_semaphore()

    def greet(p, c):
        pl.semaphore_signal(
            barrier, inc=1, device_id={"sp": (me + p) % n}, device_id_type=MESH
        )
        return c

    lax.fori_loop(1, n, greet, 0)
    for other in (mate, partner, across):
        pl.semaphore_signal(barrier, inc=1, device_id={"tp": other}, device_id_type=MESH)
    pl.semaphore_wait(barrier, n + 2)

    def remote(src, dst, s, r, dev):
        return pltpu.make_async_remote_copy(
            src_ref=src, dst_ref=dst, send_sem=s, recv_sem=r, device_id=dev, device_id_type=MESH
        )

    def span(p):
        return pl.ds(pl.multiple_of(p * cap, cap), cap)

    def span_g(i):
        return pl.ds(pl.multiple_of(i * rows, rows), rows)

    def a2a(p):
        return remote(
            outgoing.at[(me + p) % n],
            arrived.at[t, span(p)],
            a2a_s.at[p],
            a2a_r.at[p],
            {"sp": (me + p) % n},
        )

    def slab(p):
        return arrived.at[t, span(p)]

    def agy(p):
        return remote(slab(p), slab(p), agy_s.at[p], agy_r.at[p], {"tp": partner})

    def agm(p):
        return remote(slab(p), slab(p), agm_s.at[p], agm_r.at[p], {"tp": mate})

    def agf(p):
        piece = arrived.at[partner, span(p)]
        return remote(piece, piece, agf_s.at[p], agf_r.at[p], {"tp": mate})

    def rsm(i, h):
        return remote(
            msend.at[i, h], mrecv.at[i, h], rsm_s.at[i, h], rsm_r.at[i, h], {"tp": mate}
        )

    def rsy(p):
        return remote(
            ysend.at[span(p)], yrecv.at[span(p)], rsy_s.at[p], rsy_r.at[p], {"tp": partner}
        )

    def ret(p):
        return remote(
            rsend.at[span(p)],
            returned.at[span(me)],
            ret_s.at[p],
            ret_r.at[p],
            {"sp": (me + n - p) % n},
        )

    def each(low, high, f):
        def one(p, c):
            f(p)
            return c

        lax.fori_loop(low, high, one, 0)

    others = (mate, partner, across)

    @pl.when(me == 0)
    def _():
        halo_conv[...] = jnp.zeros_like(halo_conv)
        halo_inner[...] = jnp.zeros_like(halo_inner)
        halo_docs[...] = jnp.full_like(halo_docs, -1)

    def halo(j):
        last = pl.ds(tokens - 16, 16)
        src = (conv_input.at[last], inner_gate.at[last], documents)[j]
        dst = (halo_conv, halo_inner, halo_docs)[j]
        return remote(src, dst, halo_s.at[j], halo_r.at[j], {"sp": (me + 1) % n})

    @pl.when(me < n - 1)
    def _():
        for j in range(3):
            halo(j).start()

    f32, bf = jnp.float32, jnp.bfloat16
    row_id = lax.broadcasted_iota(jnp.int32, (tokens, tokens), 0)
    col_id = lax.broadcasted_iota(jnp.int32, (tokens, tokens), 1)
    eye = row_id == col_id

    def to_column(row):
        return jnp.sum(jnp.where(eye, row, 0.0), axis=1, keepdims=True)

    def to_row(column):
        return jnp.sum(jnp.where(eye, column, 0.0), axis=0, keepdims=True)

    expert_id = lax.broadcasted_iota(jnp.int32, (n, tokens), 0)
    hot = [(expert_id == routes[k : k + 1, :]).astype(f32) for k in range(2)]
    before = (row_id < col_id).astype(bf)
    counts = jnp.dot((hot[0] + hot[1]).astype(bf), before, preferred_element_type=f32)
    slots = [
        jnp.sum(hot[k] * (counts + (expert_id * cap).astype(f32)), axis=0, keepdims=True)
        for k in range(2)
    ]
    slot_rows = [s.astype(jnp.int32) for s in slots]
    slot_cols = [to_column(s).astype(jnp.int32) for s in slots]

    own = (inner_gate[...].astype(f32) * conv_input[...].astype(f32)).astype(bf).astype(f32)
    joined[pl.ds(16, tokens), :] = own
    doc_col = to_column(documents[...].astype(f32))
    joined_docs[pl.ds(16, tokens), :] = jnp.broadcast_to(doc_col, (tokens, chans))

    @pl.when(me > 0)
    def _():
        for j in range(3):
            halo(j).wait_recv()

    joined[pl.ds(0, 16), :] = (
        (halo_inner[...].astype(f32) * halo_conv[...].astype(f32)).astype(bf).astype(f32)
    )
    halo_col = to_column(halo_docs[...].astype(f32))
    joined_docs[pl.ds(0, 16), :] = jnp.broadcast_to(halo_col[tokens - 16 :, :], (16, chans))
    docs_here = joined_docs[pl.ds(16, tokens), :]
    same_one = (joined_docs[pl.ds(15, tokens), :] == docs_here).astype(f32)
    same_two = (joined_docs[pl.ds(14, tokens), :] == docs_here).astype(f32)
    conv_sum = (
        conv_taps[2:3, :] * own
        + conv_taps[1:2, :] * joined[pl.ds(15, tokens), :] * same_one
        + conv_taps[0:1, :] * joined[pl.ds(14, tokens), :] * same_two
    )
    mixbuf[t] = (outer_gate[...].astype(f32) * conv_sum).astype(bf)

    def mix(j):
        return remote(
            mixbuf.at[t], mixbuf.at[t], mix_s.at[j], mix_r.at[j], {"tp": others[j]}
        )

    for j in (1, 2, 0):
        mix(j).start()
    for load in early:
        load.wait()
    for j in range(3):
        mix(j).wait_recv()
    accum = None
    squares = None
    for q in range(4):
        piece = mixbuf[q].astype(f32)
        deep = slice(q * chans, (q + 1) * chans)
        scaled = (piece * mixer_gain[0:1, deep]).astype(bf)
        part = jnp.dot(scaled, ow[deep, :], preferred_element_type=f32)
        square = jnp.sum(piece * piece, axis=1, keepdims=True)
        accum = part if accum is None else accum + part
        squares = square if squares is None else squares + square
    mix_scale = lax.rsqrt(squares / (4 * chans) + EPS)
    hidden[...] = residual[...].astype(f32) + accum * mix_scale
    state = hidden[...]
    total = to_row(jnp.sum(state * state, axis=1, keepdims=True))
    totals[t] = jnp.broadcast_to(total, (8, tokens))

    def tot(j):
        return remote(
            totals.at[t], totals.at[t], tot_s.at[j], tot_r.at[j], {"tp": others[j]}
        )

    for j in (1, 2, 0):
        tot(j).start()
    for j in range(3):
        tot(j).wait_recv()
    feature_total = to_column((totals[0] + totals[1] + totals[2] + totals[3])[0:1, :])
    normed[...] = (
        hidden[...] * lax.rsqrt(feature_total / (4 * lf) + EPS) * ffn_gain[...]
    ).astype(bf)

    def pick_for(e):
        slot_id = lax.broadcasted_iota(jnp.int32, (cap, tokens), 0) + e * cap
        pick = (slot_id == slot_rows[0]) | (slot_id == slot_rows[1])
        return jnp.dot(
            pick.astype(f32).astype(bf), normed[...], preferred_element_type=f32
        ).astype(bf)

    def dispatch(p):
        e = (me + p) % n
        outgoing[e] = pick_for(e)
        a2a(p).start()

    each(1, n, dispatch)
    arrived[t, pl.ds(0, cap), :] = pick_for(me)

    def spread(p):
        @pl.when(p > 0)
        def _():
            a2a(p).wait_recv()

        agy(p).start()
        agm(p).start()

    def relay(p):
        agy(p).wait_recv()
        agf(p).start()

    def settle(p):
        agm(p).wait_recv()
        agf(p).wait_recv()

    def over_group(i, f):
        each(i * group, (i + 1) * group, f)

    def reduce_mate(i):
        rsm(i, 0).wait_recv()
        ysend[span_g(i), :] = (mine[0] + mrecv[i, 0].astype(jnp.float32)).astype(jnp.bfloat16)
        over_group(i, lambda p: rsy(p).start())
        rsm(i, 1).wait_recv()
        mine2[...] = mine[1] + mrecv[i, 1].astype(jnp.float32)

    def reduce_partner(i):
        def back(p):
            rsy(p).wait_recv()
            local = pl.ds(pl.multiple_of((p - i * group) * cap, cap), cap)
            rsend[span(p), :] = (
                mine2[local, :] + yrecv[span(p), :].astype(jnp.float32)
            ).astype(jnp.bfloat16)

            @pl.when(p > 0)
            def _():
                ret(p).start()

        over_group(i, back)

    def compute(i):
        def hidden_tile(j, c):
            cols = pl.ds(pl.multiple_of(j * 128, 128), 128)
            both = None
            for q in range(4):
                deep = slice(q * lf, (q + 1) * lf)
                w = jnp.concatenate([wg[deep, cols], wu[deep, cols]], axis=1)
                part = jnp.dot(arrived[q, span_g(i), :], w, preferred_element_type=jnp.float32)
                both = part if both is None else both + part
            g = both[:, :128]
            act[:, cols] = (g * jax.nn.sigmoid(g) * both[:, 128:]).astype(jnp.bfloat16)
            return c

        lax.fori_loop(0, units // 128, hidden_tile, 0)
        for h in range(2):
            qa = (1 - a) if h == 0 else a
            far = pl.ds(pl.multiple_of((2 * qa + 1 - b) * lf, lf), lf)
            near = pl.ds(pl.multiple_of((2 * qa + b) * lf, lf), lf)
            msend[i, h] = jnp.dot(
                act[...], wd[:, far], preferred_element_type=jnp.float32
            ).astype(jnp.bfloat16)
            rsm(i, h).start()
            mine[h] = jnp.dot(act[...], wd[:, near], preferred_element_type=jnp.float32)

    over_group(0, spread)
    if steps > 1:
        over_group(1, spread)
    for load in loads:
        load.wait()

    def step(i, c):
        over_group(i, relay)

        @pl.when(i > 0)
        def _():
            reduce_mate(i - 1)

        over_group(i, settle)

        @pl.when(i + 2 < steps)
        def _():
            over_group(i + 2, spread)

        compute(i)

        @pl.when(i > 0)
        def _():
            reduce_partner(i - 1)

        return c

    lax.fori_loop(0, steps, step, 0)
    reduce_mate(steps - 1)
    reduce_partner(steps - 1)
    returned[span(me), :] = rsend[pl.ds(0, cap), :]
    each(1, n, lambda p: ret(p).wait_recv())

    weight_cols = [to_column(route_weights[k : k + 1, :]) for k in range(2)]
    layer = hidden[...]
    for i in range(steps):
        here = returned[i * rows : (i + 1) * rows, :]
        slot_id = lax.broadcasted_iota(jnp.int32, (tokens, rows), 1) + i * rows
        for k in range(2):
            pick = (slot_id == slot_cols[k]).astype(f32).astype(bf)
            picked = jnp.dot(pick, here, preferred_element_type=f32)
            layer = layer + picked * weight_cols[k]
    layer_out[...] = layer.astype(bf)

    def finish(p):
        agy(p).wait_send()
        agm(p).wait_send()
        agf(p).wait_send()

        @pl.when(p > 0)
        def _():
            a2a(p).wait_send()
            ret(p).wait_send()

    each(0, n, finish)

    each(0, n, lambda p: rsy(p).wait_send())

    def finish_group(i):
        rsm(i, 0).wait_send()
        rsm(i, 1).wait_send()

    each(0, steps, finish_group)
    for j in range(3):
        mix(j).wait_send()
        tot(j).wait_send()

    @pl.when(me < n - 1)
    def _():
        for j in range(3):
            halo(j).wait_send()


def per_device(
    residual_in,
    conv_input,
    outer_gate,
    inner_gate,
    documents,
    conv_taps,
    mixer_gain,
    output_weight,
    ffn_gain,
    routes,
    route_weights,
    expert_gate,
    expert_up,
    expert_down,
):
    tokens, lf = residual_in.shape
    chans = conv_input.shape[1]
    n = lax.axis_size("sp") * expert_gate.shape[0]
    cap = 4 * tokens // n
    width, units = expert_gate.shape[1:]
    group = max(1, min(n, 256 // cap))
    rows, steps = group * cap, n // group
    bf, f32 = jnp.bfloat16, jnp.float32
    dma = pltpu.SemaphoreType.DMA
    vmem, hbm = pl.BlockSpec(memory_space=pltpu.VMEM), pl.BlockSpec(memory_space=pl.ANY)
    return pl.pallas_call(
        functools.partial(layer_kernel, n, group),
        out_shape=jax.ShapeDtypeStruct((tokens, lf), bf),
        in_specs=[hbm] + [vmem] * 6 + [hbm] + [vmem] * 3 + [hbm] * 3,
        out_specs=vmem,
        scratch_shapes=[
            pltpu.VMEM((tokens, lf), bf),
            pltpu.VMEM(output_weight.shape, bf),
            pltpu.VMEM((16, chans), bf),
            pltpu.VMEM((16, chans), bf),
            pltpu.VMEM((1, tokens), jnp.int32),
            pltpu.VMEM((tokens + 16, chans), f32),
            pltpu.VMEM((tokens + 16, chans), f32),
            pltpu.VMEM((4, tokens, chans), bf),
            pltpu.VMEM((4, 8, tokens), f32),
            pltpu.VMEM((tokens, lf), f32),
            pltpu.VMEM((tokens, lf), bf),
            pltpu.VMEM((n, cap, lf), bf),
            pltpu.VMEM((n * cap, lf), bf),
            pltpu.VMEM((width, units), bf),
            pltpu.VMEM((width, units), bf),
            pltpu.VMEM((units, width), bf),
            pltpu.VMEM((4, n * cap, lf), bf),
            pltpu.VMEM((rows, units), bf),
            pltpu.VMEM((steps, 2, rows, lf), bf),
            pltpu.VMEM((steps, 2, rows, lf), bf),
            pltpu.VMEM((2, rows, lf), f32),
            pltpu.VMEM((n * cap, lf), bf),
            pltpu.VMEM((n * cap, lf), bf),
            pltpu.VMEM((rows, lf), f32),
            pltpu.VMEM((n * cap, lf), bf),
            dma((5,)),
        ]
        + [dma((n,))] * 8
        + [dma((steps, 2))] * 2
        + [dma((n,))] * 4
        + [dma((3,))] * 6,
        compiler_params=pltpu.CompilerParams(
            collective_id=0, has_side_effects=True, vmem_limit_bytes=58 * 1024 * 1024
        ),
        name="layer",
    )(
        residual_in,
        conv_input,
        outer_gate,
        inner_gate,
        documents.reshape(1, tokens),
        conv_taps,
        mixer_gain.reshape(1, -1),
        output_weight,
        ffn_gain.reshape(1, -1),
        routes.T,
        route_weights.T,
        expert_gate,
        expert_up,
        expert_down,
    )


def solution(mesh):
    placed = (
        P("sp", "tp"),
        P("sp", "tp"),
        P("sp", "tp"),
        P("sp", "tp"),
        P("sp"),
        P(None, "tp"),
        P(),
        P(None, "tp"),
        P("tp"),
        P("sp", None),
        P("sp", None),
        P("sp", None, "tp"),
        P("sp", None, "tp"),
        P("sp", "tp", None),
    )
    return jax.shard_map(
        per_device, mesh=mesh, in_specs=placed, out_specs=P("sp", "tp"), check_vma=False
    )
```

```python
import functools

import jax
import jax.numpy as jnp
from jax import lax
from jax.experimental import pallas as pl
from jax.experimental.pallas import tpu as pltpu
from jax.sharding import PartitionSpec as P

EPS = 1e-06
MESH = pl.DeviceIdType.MESH


def layer_kernel(
    n,
    group,
    residual_hbm,
    conv_input,
    outer_gate,
    inner_gate,
    documents,
    conv_taps,
    mixer_gain,
    ow_hbm,
    ffn_gain,
    routes,
    route_weights,
    gate_hbm,
    up_hbm,
    down_hbm,
    layer_out,
    residual,
    ow,
    halo_conv,
    halo_inner,
    halo_docs,
    joined,
    joined_docs,
    mixbuf,
    totals,
    hidden,
    normed,
    outgoing,
    returned,
    wg,
    wu,
    wd,
    arrived,
    act,
    msend,
    mrecv,
    mine,
    ysend,
    yrecv,
    mine2,
    rsend,
    w_sem,
    a2a_s,
    a2a_r,
    agy_s,
    agy_r,
    agm_s,
    agm_r,
    agf_s,
    agf_r,
    rsm_s,
    rsm_r,
    rsy_s,
    rsy_r,
    ret_s,
    ret_r,
    halo_s,
    halo_r,
    mix_s,
    mix_r,
    tot_s,
    tot_r,
):
    me = lax.axis_index("sp")
    t = lax.axis_index("tp")
    a = t // 2
    b = t % 2
    mate = 2 * a + (1 - b)
    partner = 2 * (1 - a) + b
    across = 2 * (1 - a) + (1 - b)
    cap, lf = outgoing.shape[1], outgoing.shape[2]
    units = wg.shape[1]
    tokens = conv_input.shape[0]
    chans = conv_input.shape[1]
    rows = group * cap
    steps = n // group

    early = [
        pltpu.make_async_copy(ow_hbm, ow, w_sem.at[3]),
        pltpu.make_async_copy(residual_hbm, residual, w_sem.at[4]),
    ]
    loads = [
        pltpu.make_async_copy(gate_hbm.at[0], wg, w_sem.at[0]),
        pltpu.make_async_copy(up_hbm.at[0], wu, w_sem.at[1]),
        pltpu.make_async_copy(down_hbm.at[0], wd, w_sem.at[2]),
    ]
    for load in early + loads:
        load.start()

    barrier = pltpu.get_barrier_semaphore()

    def greet(p, c):
        pl.semaphore_signal(
            barrier, inc=1, device_id={"sp": (me + p) % n}, device_id_type=MESH
        )
        return c

    lax.fori_loop(1, n, greet, 0)
    for other in (mate, partner, across):
        pl.semaphore_signal(barrier, inc=1, device_id={"tp": other}, device_id_type=MESH)
    pl.semaphore_wait(barrier, n + 2)

    def remote(src, dst, s, r, dev):
        return pltpu.make_async_remote_copy(
            src_ref=src, dst_ref=dst, send_sem=s, recv_sem=r, device_id=dev, device_id_type=MESH
        )

    def span(p):
        return pl.ds(pl.multiple_of(p * cap, cap), cap)

    def span_g(i):
        return pl.ds(pl.multiple_of(i * rows, rows), rows)

    def a2a(p):
        return remote(
            outgoing.at[(me + p) % n],
            arrived.at[t, span(p)],
            a2a_s.at[p],
            a2a_r.at[p],
            {"sp": (me + p) % n},
        )

    def slab(p):
        return arrived.at[t, span(p)]

    def agy(p):
        return remote(slab(p), slab(p), agy_s.at[p], agy_r.at[p], {"tp": partner})

    def agm(p):
        return remote(slab(p), slab(p), agm_s.at[p], agm_r.at[p], {"tp": mate})

    def agf(p):
        piece = arrived.at[partner, span(p)]
        return remote(piece, piece, agf_s.at[p], agf_r.at[p], {"tp": mate})

    def rsm(i, h):
        return remote(
            msend.at[i, h], mrecv.at[i, h], rsm_s.at[i, h], rsm_r.at[i, h], {"tp": mate}
        )

    def rsy(p):
        return remote(
            ysend.at[span(p)], yrecv.at[span(p)], rsy_s.at[p], rsy_r.at[p], {"tp": partner}
        )

    def ret(p):
        return remote(
            rsend.at[span(p)],
            returned.at[span(p)],
            ret_s.at[p],
            ret_r.at[p],
            {"sp": (me + n - p) % n},
        )

    def each(low, high, f):
        def one(p, c):
            f(p)
            return c

        lax.fori_loop(low, high, one, 0)

    others = (mate, partner, across)

    @pl.when(me == 0)
    def _():
        halo_conv[...] = jnp.zeros_like(halo_conv)
        halo_inner[...] = jnp.zeros_like(halo_inner)
        halo_docs[...] = jnp.full_like(halo_docs, -1)

    def halo(j):
        last = pl.ds(tokens - 16, 16)
        src = (conv_input.at[last], inner_gate.at[last], documents)[j]
        dst = (halo_conv, halo_inner, halo_docs)[j]
        return remote(src, dst, halo_s.at[j], halo_r.at[j], {"sp": (me + 1) % n})

    @pl.when(me < n - 1)
    def _():
        for j in range(3):
            halo(j).start()

    f32, bf = jnp.float32, jnp.bfloat16
    row_id = lax.broadcasted_iota(jnp.int32, (tokens, tokens), 0)
    col_id = lax.broadcasted_iota(jnp.int32, (tokens, tokens), 1)
    eye = row_id == col_id

    def to_column(row):
        return jnp.sum(jnp.where(eye, row, 0.0), axis=1, keepdims=True)

    def to_row(column):
        return jnp.sum(jnp.where(eye, column, 0.0), axis=0, keepdims=True)

    expert_id = lax.broadcasted_iota(jnp.int32, (n, tokens), 0)
    hot = [(expert_id == routes[k : k + 1, :]).astype(f32) for k in range(2)]
    before = (row_id < col_id).astype(bf)
    counts = jnp.dot((hot[0] + hot[1]).astype(bf), before, preferred_element_type=f32)
    slots = [
        jnp.sum(hot[k] * (counts + (expert_id * cap).astype(f32)), axis=0, keepdims=True)
        for k in range(2)
    ]
    slot_rows = [s.astype(jnp.int32) for s in slots]
    slot_cols = []
    for s in slots:
        near = s.astype(jnp.int32) - me * cap
        near = jnp.where(near < 0, near + n * cap, near)
        slot_cols.append(to_column(near.astype(f32)).astype(jnp.int32))

    own = (inner_gate[...].astype(f32) * conv_input[...].astype(f32)).astype(bf).astype(f32)
    joined[pl.ds(16, tokens), :] = own
    doc_col = to_column(documents[...].astype(f32))
    joined_docs[pl.ds(16, tokens), :] = jnp.broadcast_to(doc_col, (tokens, chans))

    @pl.when(me > 0)
    def _():
        for j in range(3):
            halo(j).wait_recv()

    joined[pl.ds(0, 16), :] = (
        (halo_inner[...].astype(f32) * halo_conv[...].astype(f32)).astype(bf).astype(f32)
    )
    halo_col = to_column(halo_docs[...].astype(f32))
    joined_docs[pl.ds(0, 16), :] = jnp.broadcast_to(halo_col[tokens - 16 :, :], (16, chans))
    docs_here = joined_docs[pl.ds(16, tokens), :]
    same_one = (joined_docs[pl.ds(15, tokens), :] == docs_here).astype(f32)
    same_two = (joined_docs[pl.ds(14, tokens), :] == docs_here).astype(f32)
    conv_sum = (
        conv_taps[2:3, :] * own
        + conv_taps[1:2, :] * joined[pl.ds(15, tokens), :] * same_one
        + conv_taps[0:1, :] * joined[pl.ds(14, tokens), :] * same_two
    )
    mixbuf[t] = (outer_gate[...].astype(f32) * conv_sum).astype(bf)

    def mix(j):
        return remote(
            mixbuf.at[t], mixbuf.at[t], mix_s.at[j], mix_r.at[j], {"tp": others[j]}
        )

    for j in (1, 2, 0):
        mix(j).start()
    for load in early:
        load.wait()
    for j in range(3):
        mix(j).wait_recv()
    accum = None
    squares = None
    for q in range(4):
        piece = mixbuf[q].astype(f32)
        deep = slice(q * chans, (q + 1) * chans)
        scaled = (piece * mixer_gain[0:1, deep]).astype(bf)
        part = jnp.dot(scaled, ow[deep, :], preferred_element_type=f32)
        square = jnp.sum(piece * piece, axis=1, keepdims=True)
        accum = part if accum is None else accum + part
        squares = square if squares is None else squares + square
    mix_scale = lax.rsqrt(squares / (4 * chans) + EPS)
    hidden[...] = residual[...].astype(f32) + accum * mix_scale
    state = hidden[...]
    total = to_row(jnp.sum(state * state, axis=1, keepdims=True))
    totals[t] = jnp.broadcast_to(total, (8, tokens))

    def tot(j):
        return remote(
            totals.at[t], totals.at[t], tot_s.at[j], tot_r.at[j], {"tp": others[j]}
        )

    for j in (1, 2, 0):
        tot(j).start()
    for j in range(3):
        tot(j).wait_recv()
    feature_total = to_column((totals[0] + totals[1] + totals[2] + totals[3])[0:1, :])
    normed[...] = (
        hidden[...] * lax.rsqrt(feature_total / (4 * lf) + EPS) * ffn_gain[...]
    ).astype(bf)

    def pick_for(e):
        slot_id = lax.broadcasted_iota(jnp.int32, (cap, tokens), 0) + e * cap
        pick = (slot_id == slot_rows[0]) | (slot_id == slot_rows[1])
        return jnp.dot(
            pick.astype(f32).astype(bf), normed[...], preferred_element_type=f32
        ).astype(bf)

    def dispatch(p):
        e = (me + p) % n
        outgoing[e] = pick_for(e)
        a2a(p).start()

    arrived[t, pl.ds(0, cap), :] = pick_for(me)
    agy(0).start()
    agm(0).start()
    each(1, n, dispatch)

    def spread(p):
        a2a(p).wait_recv()
        agy(p).start()
        agm(p).start()

    def relay(p):
        agy(p).wait_recv()
        agf(p).start()

    def settle(p):
        agm(p).wait_recv()
        agf(p).wait_recv()

    def over_group(i, f):
        each(i * group, (i + 1) * group, f)

    def reduce_mate(i):
        rsm(i, 0).wait_recv()
        ysend[span_g(i), :] = (mine[0] + mrecv[i, 0].astype(jnp.float32)).astype(jnp.bfloat16)
        over_group(i, lambda p: rsy(p).start())
        rsm(i, 1).wait_recv()
        mine2[...] = mine[1] + mrecv[i, 1].astype(jnp.float32)

    def reduce_partner(i):
        def back(p):
            rsy(p).wait_recv()
            local = pl.ds(pl.multiple_of((p - i * group) * cap, cap), cap)
            rsend[span(p), :] = (
                mine2[local, :] + yrecv[span(p), :].astype(jnp.float32)
            ).astype(jnp.bfloat16)

            @pl.when(p > 0)
            def _():
                ret(p).start()

        over_group(i, back)

    def compute(i):
        whole = jnp.concatenate([arrived[q, span_g(i), :] for q in range(4)], axis=1)
        for j in range(units // 128):
            cols = slice(j * 128, (j + 1) * 128)
            w = jnp.concatenate([wg[:, cols], wu[:, cols]], axis=1)
            both = jnp.dot(whole, w, preferred_element_type=jnp.float32)
            g = both[:, :128]
            act[:, cols] = (g * jax.nn.sigmoid(g) * both[:, 128:]).astype(jnp.bfloat16)
        for h in range(2):
            qa = (1 - a) if h == 0 else a
            far = pl.ds(pl.multiple_of((2 * qa + 1 - b) * lf, lf), lf)
            near = pl.ds(pl.multiple_of((2 * qa + b) * lf, lf), lf)
            msend[i, h] = jnp.dot(
                act[...], wd[:, far], preferred_element_type=jnp.float32
            ).astype(jnp.bfloat16)
            rsm(i, h).start()
            mine[h] = jnp.dot(act[...], wd[:, near], preferred_element_type=jnp.float32)

    each(1, group, spread)
    if steps > 1:
        over_group(1, spread)
    for load in loads:
        load.wait()

    def step(i, c):
        over_group(i, relay)

        @pl.when(i > 0)
        def _():
            reduce_mate(i - 1)

        over_group(i, settle)

        @pl.when(i + 2 < steps)
        def _():
            over_group(i + 2, spread)

        compute(i)

        @pl.when(i > 0)
        def _():
            reduce_partner(i - 1)

        return c

    lax.fori_loop(0, steps, step, 0)
    reduce_mate(steps - 1)

    weight_cols = [to_column(route_weights[k : k + 1, :]) for k in range(2)]

    def combine(i):
        def came(p):
            @pl.when(p > 0)
            def _():
                ret(p).wait_recv()

        over_group(i, came)
        if i == 0:
            here = jnp.concatenate(
                [rsend[0:cap, :], returned[cap:rows, :]], axis=0
            ) if group > 1 else rsend[0:cap, :]
        else:
            here = returned[i * rows : (i + 1) * rows, :]
        slot_id = lax.broadcasted_iota(jnp.int32, (tokens, rows), 1) + i * rows
        total = hidden[...]
        for k in range(2):
            pick = (slot_id == slot_cols[k]).astype(f32).astype(bf)
            picked = jnp.dot(pick, here, preferred_element_type=f32)
            total = total + picked * weight_cols[k]
        return total

    for i in range(steps - 2):
        hidden[...] = combine(i)
    reduce_partner(steps - 1)
    for i in range(max(0, steps - 2), steps - 1):
        hidden[...] = combine(i)
    layer_out[...] = combine(steps - 1).astype(bf)


    def finish(p):
        agy(p).wait_send()
        agm(p).wait_send()
        agf(p).wait_send()

        @pl.when(p > 0)
        def _():
            a2a(p).wait_send()
            ret(p).wait_send()

    each(0, n, finish)

    each(0, n, lambda p: rsy(p).wait_send())

    def finish_group(i):
        rsm(i, 0).wait_send()
        rsm(i, 1).wait_send()

    each(0, steps, finish_group)
    for j in range(3):
        mix(j).wait_send()
        tot(j).wait_send()

    @pl.when(me < n - 1)
    def _():
        for j in range(3):
            halo(j).wait_send()


def per_device(
    residual_in,
    conv_input,
    outer_gate,
    inner_gate,
    documents,
    conv_taps,
    mixer_gain,
    output_weight,
    ffn_gain,
    routes,
    route_weights,
    expert_gate,
    expert_up,
    expert_down,
):
    tokens, lf = residual_in.shape
    chans = conv_input.shape[1]
    n = lax.axis_size("sp") * expert_gate.shape[0]
    cap = 4 * tokens // n
    width, units = expert_gate.shape[1:]
    group = max(1, min(n, 256 // cap))
    rows, steps = group * cap, n // group
    bf, f32 = jnp.bfloat16, jnp.float32
    dma = pltpu.SemaphoreType.DMA
    vmem, hbm = pl.BlockSpec(memory_space=pltpu.VMEM), pl.BlockSpec(memory_space=pl.ANY)
    return pl.pallas_call(
        functools.partial(layer_kernel, n, group),
        out_shape=jax.ShapeDtypeStruct((tokens, lf), bf),
        in_specs=[hbm] + [vmem] * 6 + [hbm] + [vmem] * 3 + [hbm] * 3,
        out_specs=vmem,
        scratch_shapes=[
            pltpu.VMEM((tokens, lf), bf),
            pltpu.VMEM(output_weight.shape, bf),
            pltpu.VMEM((16, chans), bf),
            pltpu.VMEM((16, chans), bf),
            pltpu.VMEM((1, tokens), jnp.int32),
            pltpu.VMEM((tokens + 16, chans), f32),
            pltpu.VMEM((tokens + 16, chans), f32),
            pltpu.VMEM((4, tokens, chans), bf),
            pltpu.VMEM((4, 8, tokens), f32),
            pltpu.VMEM((tokens, lf), f32),
            pltpu.VMEM((tokens, lf), bf),
            pltpu.VMEM((n, cap, lf), bf),
            pltpu.VMEM((n * cap, lf), bf),
            pltpu.VMEM((width, units), bf),
            pltpu.VMEM((width, units), bf),
            pltpu.VMEM((units, width), bf),
            pltpu.VMEM((4, n * cap, lf), bf),
            pltpu.VMEM((rows, units), bf),
            pltpu.VMEM((steps, 2, rows, lf), bf),
            pltpu.VMEM((steps, 2, rows, lf), bf),
            pltpu.VMEM((2, rows, lf), f32),
            pltpu.VMEM((n * cap, lf), bf),
            pltpu.VMEM((n * cap, lf), bf),
            pltpu.VMEM((rows, lf), f32),
            pltpu.VMEM((n * cap, lf), bf),
            dma((5,)),
        ]
        + [dma((n,))] * 8
        + [dma((steps, 2))] * 2
        + [dma((n,))] * 4
        + [dma((3,))] * 6,
        compiler_params=pltpu.CompilerParams(
            collective_id=0, has_side_effects=True, vmem_limit_bytes=58 * 1024 * 1024
        ),
        name="layer",
    )(
        residual_in,
        conv_input,
        outer_gate,
        inner_gate,
        documents.reshape(1, tokens),
        conv_taps,
        mixer_gain.reshape(1, -1),
        output_weight,
        ffn_gain.reshape(1, -1),
        routes.T,
        route_weights.T,
        expert_gate,
        expert_up,
        expert_down,
    )


def solution(mesh):
    placed = (
        P("sp", "tp"),
        P("sp", "tp"),
        P("sp", "tp"),
        P("sp", "tp"),
        P("sp"),
        P(None, "tp"),
        P(),
        P(None, "tp"),
        P("tp"),
        P("sp", None),
        P("sp", None),
        P("sp", None, "tp"),
        P("sp", None, "tp"),
        P("sp", "tp", None),
    )
    return jax.shard_map(
        per_device, mesh=mesh, in_specs=placed, out_specs=P("sp", "tp"), check_vma=False
    )
```
